32 devices in a mesh: ep: 8 (over z, y), tp: 4 (over x, core).
Axes of the slice: x: 2, y: 2, z: 4, core: 2. Of those that a mesh axis runs over, the one named last changes fastest.
Arguments:
- query: bfloat16 [1024, 1536], P('ep', 'tp'), may hold values from -136 to 136
- latent: bfloat16 [1024, 512], P(('ep', 'tp')), may hold values from -6 to 6
- rope_key: bfloat16 [1024, 32], P(('ep', 'tp')), may hold values from -6 to 6
- latent_gain: float32 [512], replicated, may hold values from 0.1 to 1.9
- key_up: bfloat16 [512, 1024], P(None, 'tp'), may hold values from -0.25 to 0.25
- value_up: bfloat16 [512, 1024], P(None, 'tp'), may hold values from -2 to 2
- out_proj: bfloat16 [1024, 2048], replicated, may hold values from -0.1875 to 0.1875
- tokens: bfloat16 [2048, 2048], P(('ep', 'tp')), may hold values from -6 to 6
- moe_gain: float32 [2048], replicated, may hold values from 0.1 to 1.9
- routes: int32 [2048, 2], P(('ep', 'tp')), may hold values from 0 to 7, all different within a row; in each aligned block of 64 rows (0 to 63, 64 to 127, ...) at most 32 rows name the same one
- group_prob: float32 [2048], P(('ep', 'tp')), may hold values from 0.25 to 1
- expert_prob: float32 [2048, 2], P(('ep', 'tp')), may hold values from 0.02 to 1
- w_gate: bfloat16 [8, 2048, 1024], P('ep', None, 'tp'), may hold values from -0.125 to 0.125
- w_up: bfloat16 [8, 2048, 1024], P('ep', None, 'tp'), may hold values from -0.125 to 0.125
- w_down: bfloat16 [8, 1024, 2048], P('ep', 'tp'), may hold values from -0.1875 to 0.1875
Outputs:
- mixed: bfloat16 [1024, 2048], P(('ep', 'tp'))
- moe_out: bfloat16 [2048, 2048], P(('ep', 'tp'))
The draws below stay inside these ranges and needn't reach their ends.
Inputs may be any that keep to these rules, and one draw needn't show every extreme that they name: `routes`: each row names 2 different experts; within the rows of one device no expert is named more than 32 times.
All inputs are finite; a program needn't handle non-finite values.
Results may differ from the reference program's by a relative error of at most 0.025.
Values may be sent and summed in bfloat16 or wider, within the bound.
No kernel may reach another device: no remote copies, remote signals or barrier semaphores. Data moves between devices by JAX's collectives and lax.ppermute only.
A program may use at most 128 MiB of HBM per device.

```python
import functools
import math
import jax
import jax.numpy as jnp
import numpy as np
from jax import lax

D = 2048
HEADS = 16
NOPE = 64
ROPE_DIM = 32
V_DIM = 64
LATENT = 512
EXPERT_WIDTH = 1024
TOP = 2
M_ROWS = 64
SEQ = 1024
MOE_TOKENS = 2048
EXPERTS = 8
CAP = 32
N_TP = 4


def draw_query(key, part):
    first_key = jax.random.fold_in(jax.random.fold_in(key, 11), 0)
    full_shape = (SEQ, HEADS * (NOPE + ROPE_DIM))
    values = jnp.clip(2.0 * jax.random.normal(first_key, full_shape, jnp.float32), -8.0, 8.0)
    return values.astype(jnp.bfloat16)


def block_scale(own_key, dims, cuts, smallest, top_value):
    def one(position, blocks):
        draws = jax.random.uniform(jax.random.fold_in(jax.random.fold_in(own_key, 6), position), (blocks,), jnp.float32, smallest / len(cuts), top_value / len(cuts))
        return jnp.repeat(jnp.exp(draws), dims[position] // blocks).reshape((-1,) + (1,) * (len(dims) - position - 1))

    factor_of = one(*cuts[0])
    for cut in cuts[1:]:
        factor_of = factor_of * one(*cut)
    return factor_of


def assign_block(stream_key, own, number, rows, count, top, most, slope):
    order = jax.random.permutation(stream_key, count)
    crowded, usual = portions_of(count, rows * top, most, slope, True), portions_of(count, rows * top, most, slope, False)
    places = jnp.arange(count)

    def named(lengths, turn):
        used = int((lengths > 0).sum())
        fixed = max(1, used // 4)
        shifted = fixed + (places - fixed + turn * (used - fixed)) % max(1, count - fixed)
        return jnp.zeros((count,), jnp.int32).at[order[jnp.where(places < fixed, places, shifted)]].set(jnp.asarray(lengths, jnp.int32))

    lengths = jnp.where(number % 4 == 0, named(crowded, number // 4), named(usual, number - number // 4 - 1))
    mixed = jax.random.permutation(jax.random.fold_in(own, 3), count)
    source_of, taker = mixed[0:count // 2 * 2:2], mixed[1:count // 2 * 2:2]
    room = jnp.minimum(lengths[source_of] - 1, most - lengths[taker]) // 2
    room = jnp.where((source_of == order[0]) | (taker == order[0]) | (lengths[taker] == 0), 0, jnp.maximum(room, 0))
    shifted = jax.random.randint(jax.random.fold_in(own, 4), (count // 2,), 0, 1 << 20) % (room + 1)
    lengths = lengths.at[source_of].add(-shifted).at[taker].add(shifted)
    items = jnp.searchsorted(jnp.cumsum(lengths), jnp.arange(rows * top), side="right").astype(jnp.int32)
    grid = items.reshape(top, rows).T
    grid = grid[jax.random.permutation(jax.random.fold_in(own, 1), rows)]
    turn = jax.random.randint(jax.random.fold_in(own, 2), (rows, 1), 0, top)
    return jnp.take_along_axis(grid, (jnp.arange(top)[None, :] + turn) % top, axis=1)


def portions_of(number_of, total, reach, slope, full):
    portions = [(1 << 20) // math.isqrt(standing ** slope) + 1 for standing in range(1, number_of + 1)]
    largest = reach if full else min(reach, max(-(-total // number_of), total * portions[0] // sum(portions)))
    least = 1 if total - largest >= number_of - 1 else 0
    given, rest = [largest] + [least] * (number_of - 1), total - largest - least * (number_of - 1)
    while rest > 0:
        movable = [i for i in range(1, number_of) if given[i] < largest] or [i for i in range(1, number_of) if given[i] < reach]
        pool, budget = sum([portions[i] for i in movable]), rest
        for i in movable:
            more = min(reach - given[i], max(1, budget * portions[i] // pool), rest)
            given[i] = given[i] + more
            rest = rest - more
    return np.array(given)


def centred(key, shape, spread, bound, cuts=(), kind=jnp.bfloat16):
    array = jax.random.normal(key, shape, jnp.float32) * spread
    if len(cuts) > 0:
        array = block_scale(key, shape, cuts, -0.22, 0.18) * array
    return jnp.clip(array, min=-bound, max=bound).astype(kind)


def setup_inputs(seed: int = 0) -> dict:
    key_list = jax.random.split(jax.random.key(seed), 16)
    query = draw_query(jax.random.fold_in(key_list[15], 71), 0)
    latent = centred(key_list[1], (SEQ, LATENT), 1.0, 6.0, ((0, 32),))
    rope_key = centred(key_list[2], (SEQ, ROPE_DIM), 1.0, 6.0, ((0, 32),))
    latent_gain = jnp.clip(1.0 + 0.18 * jax.random.normal(key_list[3], (LATENT,), jnp.float32), 0.1, 1.9)
    key_up = centred(key_list[4], (LATENT, HEADS * NOPE), LATENT ** -0.5, 0.25, ((1, 4),))
    value_up = centred(key_list[5], (LATENT, HEADS * V_DIM), (LATENT // 64) ** -0.5, 2.0, ((1, 4),))
    out_proj = centred(key_list[6], (HEADS * V_DIM, D), (HEADS * V_DIM) ** -0.5, 0.1875)
    tokens = centred(key_list[7], (MOE_TOKENS, D), 1.0, 6.0, ((0, 32),))
    moe_gain = jnp.clip(1.0 + 0.18 * jax.random.normal(key_list[8], (D,), jnp.float32), 0.1, 1.9)
    routes_keys = jax.random.split(jax.random.fold_in(key_list[9], 1), MOE_TOKENS // M_ROWS)
    routes_turns = jax.random.permutation(jax.random.fold_in(key_list[9], 3), MOE_TOKENS // M_ROWS)
    routes = jax.vmap(lambda own, number: assign_block(jax.random.fold_in(key_list[9], 2), own, number, M_ROWS, EXPERTS, TOP, CAP, 2))(routes_keys, routes_turns).reshape((MOE_TOKENS, TOP))
    group_prob = jnp.clip(jnp.exp(math.log(1.0) - 1.3862944 * jax.random.uniform(key_list[10], (MOE_TOKENS,), jnp.float32) ** block_scale(key_list[10], (MOE_TOKENS,), ((0, 32),), -0.2, 0.2)), 0.25, 1.0)
    expert_prob = jnp.clip(jnp.exp(math.log(1.0) - 3.912023 * jax.random.uniform(key_list[11], (MOE_TOKENS, TOP), jnp.float32) ** block_scale(key_list[11], (MOE_TOKENS, TOP), ((0, 32),), -0.2, 0.2)), 0.02, 1.0)
    w_gate = centred(key_list[12], (EXPERTS, D, EXPERT_WIDTH), D ** -0.5, 0.125, ((0, 8), (2, 4)))
    w_up = centred(key_list[13], (EXPERTS, D, EXPERT_WIDTH), D ** -0.5, 0.125, ((0, 8), (2, 4)))
    w_down = centred(key_list[14], (EXPERTS, EXPERT_WIDTH, D), EXPERT_WIDTH ** -0.5, 0.1875, ((0, 8), (1, 4)))
    return {"query": query, "latent": latent, "rope_key": rope_key, "latent_gain": latent_gain, "key_up": key_up, "value_up": value_up, "out_proj": out_proj, "tokens": tokens, "moe_gain": moe_gain, "routes": routes, "group_prob": group_prob, "expert_prob": expert_prob, "w_gate": w_gate, "w_up": w_up, "w_down": w_down}


epsilon = 1e-06
rope_base = 10000.0
masked_value = -1e+30

def rms_scale(values, gain):
    widened = values.astype(jnp.float32)
    return widened * lax.rsqrt(lax.optimization_barrier(jnp.mean(widened * widened, axis=-1, keepdims=True)) + epsilon) * gain.astype(jnp.float32)

def tables(positions, rope_width):
    half_width = rope_width // 2
    inverse = rope_base ** (-2.0 * jnp.arange(half_width, dtype=jnp.float32) / rope_width)
    angles = positions.astype(jnp.float32)[:, None] * inverse[None, :]
    return (jnp.cos(angles), jnp.sin(angles))

def rotate(values, cosine, sine):
    half_width = values.shape[-1] // 2
    lower = values[..., :half_width]
    upper = values[..., half_width:]
    return jnp.concatenate([lower * cosine - upper * sine, lower * sine + upper * cosine], axis=-1)

def head_attention(rope_prefix, query_pos, parts):
    query_head, key_head, value_head = parts
    full_keys = jnp.concatenate([key_head, rope_prefix], axis=-1)
    scores = jnp.dot(query_head, full_keys.T, preferred_element_type=jnp.float32) * (NOPE + ROPE_DIM) ** (-0.5)
    key_pos = jnp.arange(full_keys.shape[0], dtype=jnp.int32)
    allowed = key_pos[None, :] <= query_pos[:, None]
    scores = jnp.where(allowed, scores, masked_value)
    row_peak = lax.optimization_barrier(jnp.max(scores, axis=-1, keepdims=True))
    raised = jnp.where(allowed, jnp.exp(scores - row_peak), 0.0)
    totals = lax.optimization_barrier(jnp.sum(raised, axis=-1, keepdims=True))
    summed = jnp.dot(raised.astype(jnp.bfloat16), value_head, preferred_element_type=jnp.float32)
    return (summed / totals).astype(jnp.bfloat16)

def mixer_reference(query, latent, rope_key, latent_gain, key_up, value_up, out_proj):
    seq_len = latent.shape[0]
    positions = jnp.arange(seq_len, dtype=jnp.int32)
    cosine, sine = tables(positions, ROPE_DIM)
    normed = rms_scale(latent, latent_gain).astype(jnp.bfloat16)
    rotated_key = rotate(rope_key.astype(jnp.float32), cosine, sine).astype(jnp.bfloat16)
    query_heads = query.reshape(seq_len, HEADS, NOPE + ROPE_DIM)
    turned = rotate(query_heads[..., NOPE:].astype(jnp.float32), cosine[:, None, :], sine[:, None, :]).astype(jnp.bfloat16)
    rotated_query = jnp.concatenate([query_heads[..., :NOPE], turned], axis=-1)
    key_nope = jnp.dot(normed, key_up, preferred_element_type=jnp.float32).astype(jnp.bfloat16).reshape(seq_len, HEADS, NOPE)
    values = jnp.dot(normed, value_up, preferred_element_type=jnp.float32).astype(jnp.bfloat16).reshape(seq_len, HEADS, V_DIM)
    block_len = math.gcd(seq_len, 512)
    pieces = []
    for block_at in range(seq_len // block_len):
        upto = (block_at + 1) * block_len
        query_pos = positions[block_at * block_len:upto]
        parts = (rotated_query[block_at * block_len:upto].transpose(1, 0, 2), key_nope[:upto].transpose(1, 0, 2), values[:upto].transpose(1, 0, 2))
        result = lax.map(functools.partial(head_attention, rotated_key[:upto], query_pos), parts)
        pieces.append(result.transpose(1, 0, 2).reshape(block_len, HEADS * V_DIM))
    attention = jnp.concatenate(pieces, axis=0)
    return jnp.dot(attention, out_proj, preferred_element_type=jnp.float32).astype(jnp.bfloat16)

def expert_reference(tokens, moe_gain, routes, group_prob, expert_prob, w_gate, w_up, w_down):
    amount = tokens.shape[0]
    model_width = tokens.shape[1]
    expert_count = w_gate.shape[0]
    block_count = amount // M_ROWS
    normed = rms_scale(tokens, moe_gain).astype(jnp.bfloat16)
    flat_routes = routes.reshape(block_count, M_ROWS * TOP)
    onehot = (flat_routes[:, :, None] == jnp.arange(expert_count, dtype=jnp.int32)[None, None, :]).astype(jnp.int32)
    earlier = jnp.cumsum(onehot, axis=1) - onehot
    slot_index = lax.optimization_barrier(jnp.sum(earlier * onehot, axis=2))
    block_ids = jnp.arange(block_count, dtype=jnp.int32)[:, None]
    place = block_ids * CAP + slot_index
    source_row = block_ids * M_ROWS + jnp.arange(M_ROWS * TOP, dtype=jnp.int32)[None, :] // TOP
    shares = group_prob[:, None] * expert_prob / lax.optimization_barrier(jnp.sum(expert_prob, axis=1, keepdims=True))
    row_table = jnp.full((expert_count, block_count * CAP), amount, jnp.int32).at[flat_routes, place].set(source_row)
    share_table = jnp.zeros((expert_count, block_count * CAP), jnp.float32).at[flat_routes, place].set(shares.reshape(block_count, M_ROWS * TOP))
    padded = jnp.concatenate([normed, jnp.zeros((1, model_width), jnp.bfloat16)], axis=0)
    group_width = w_down.shape[1] // N_TP

    def per_expert(running, parts):
        row_ids, row_shares, gate_weight, up_weight, down_weight = parts
        rows_here = padded[row_ids]
        gate_values = jnp.dot(rows_here, gate_weight, preferred_element_type=jnp.float32)
        up_values = jnp.dot(rows_here, up_weight, preferred_element_type=jnp.float32)
        hidden = (jax.nn.silu(gate_values) * up_values).astype(jnp.bfloat16)
        summed = jnp.zeros((rows_here.shape[0], model_width), jnp.float32)
        for group_at in range(N_TP):
            lower_edge = group_at * group_width
            partial_low = jnp.dot(hidden[:, lower_edge:lower_edge + group_width], down_weight[lower_edge:lower_edge + group_width], preferred_element_type=jnp.float32).astype(jnp.bfloat16)
            partial_low = lax.optimization_barrier(partial_low)
            summed = summed + partial_low.astype(jnp.float32)
        expert_out = summed.astype(jnp.bfloat16)
        expert_out = lax.optimization_barrier(expert_out)
        running = running.at[row_ids].add(row_shares[:, None] * expert_out.astype(jnp.float32))
        return (running, None)
    running, _ = lax.scan(per_expert, jnp.zeros((amount + 1, model_width), jnp.float32), (row_table, share_table, w_gate, w_up, w_down))
    return running[:amount].astype(jnp.bfloat16)

def reference(query, latent, rope_key, latent_gain, key_up, value_up, out_proj, tokens, moe_gain, routes, group_prob, expert_prob, w_gate, w_up, w_down):
    mixed = mixer_reference(query, latent, rope_key, latent_gain, key_up, value_up, out_proj)
    moe_out = expert_reference(tokens, moe_gain, routes, group_prob, expert_prob, w_gate, w_up, w_down)
    return (mixed, moe_out)
```

```python
import jax
import jax.numpy as jnp
from jax import lax
from jax.experimental import pallas as pl
from jax.experimental.pallas import tpu as pltpu
from jax.sharding import PartitionSpec as P

NOPE = 64
ROPE_DIM = 32
V_DIM = 64


epsilon = 1e-06
rope_base = 10000.0
masked_value = -1e30


def rms_scale(values, gain):
    widened = values.astype(jnp.float32)
    return widened * lax.rsqrt(jnp.mean(widened * widened, axis=-1, keepdims=True) + epsilon) * gain


def tables(positions, rope_width):
    half_width = rope_width // 2
    inverse = rope_base ** (-2.0 * jnp.arange(half_width, dtype=jnp.float32) / rope_width)
    angles = positions.astype(jnp.float32)[:, None] * inverse[None, :]
    return (jnp.cos(angles), jnp.sin(angles))


def rotate(values, cosine, sine):
    half_width = values.shape[-1] // 2
    lower = values[..., :half_width]
    upper = values[..., half_width:]
    return jnp.concatenate([lower * cosine - upper * sine, lower * sine + upper * cosine], axis=-1)


def flip(value, axis, offset):
    count = lax.axis_size(axis)
    return lax.ppermute(value, axis, [(i, i ^ offset) for i in range(count)])


def attend(query, packed, key_pos, query_pos, key_up, value_up):
    query_rows = query.shape[0]
    head_count = query.shape[1] // (NOPE + ROPE_DIM)
    latent_width = key_up.shape[0]
    query_cos, query_sin = tables(query_pos, ROPE_DIM)
    query_heads = query.reshape(query_rows, head_count, NOPE + ROPE_DIM)
    turned = rotate(
        query_heads[..., NOPE:].astype(jnp.float32), query_cos[:, None, :], query_sin[:, None, :]
    ).astype(jnp.bfloat16)
    query_rot = jnp.concatenate([query_heads[..., :NOPE], turned], axis=-1)
    normed = packed[:, :latent_width]
    rope_part = packed[:, latent_width:]
    keys = jnp.dot(normed, key_up, preferred_element_type=jnp.float32).astype(jnp.bfloat16)
    values = jnp.dot(normed, value_up, preferred_element_type=jnp.float32).astype(jnp.bfloat16)
    allowed = key_pos[None, :] <= query_pos[:, None]
    scale = (NOPE + ROPE_DIM) ** (-0.5)
    pieces = []
    for head in range(head_count):
        full_keys = jnp.concatenate([keys[:, head * NOPE:(head + 1) * NOPE], rope_part], axis=1)
        scores = lax.dot_general(
            query_rot[:, head], full_keys, (((1,), (1,)), ((), ())),
            preferred_element_type=jnp.float32,
        ) * scale
        scores = jnp.where(allowed, scores, masked_value)
        top = jnp.max(scores, axis=-1, keepdims=True)
        raised = jnp.where(allowed, jnp.exp(scores - top), 0.0)
        totals = jnp.sum(raised, axis=-1, keepdims=True)
        weighted = jnp.dot(
            raised.astype(jnp.bfloat16), values[:, head * V_DIM:(head + 1) * V_DIM],
            preferred_element_type=jnp.float32,
        )
        pieces.append((weighted / totals).astype(jnp.bfloat16))
    return jnp.concatenate(pieces, axis=1)


def pack_latent(latent, rope_key, latent_gain):
    own_rows = latent.shape[0]
    start = (lax.axis_index("ep") * lax.axis_size("tp") + lax.axis_index("tp")) * own_rows
    normed = rms_scale(latent, latent_gain).astype(jnp.bfloat16)
    cosine, sine = tables(start + jnp.arange(own_rows, dtype=jnp.int32), ROPE_DIM)
    rotated = rotate(rope_key.astype(jnp.float32), cosine, sine).astype(jnp.bfloat16)
    return jnp.concatenate([normed, rotated], axis=1)


def turn(values, cosine, sine):
    width = values.shape[-1]
    half = width // 2
    row = lax.broadcasted_iota(jnp.int32, (width, width), 0)
    column = lax.broadcasted_iota(jnp.int32, (width, width), 1)
    swap = jnp.where(column < half, column + half, column - half) == row
    sign = jnp.where(column < half, -1.0, 1.0)
    swapped = jnp.dot(
        values, jnp.where(swap, sign, 0.0).astype(jnp.bfloat16),
        preferred_element_type=jnp.float32,
    )
    return (values.astype(jnp.float32) * cosine + swapped * sine).astype(jnp.bfloat16)


def dispatch_kernel(tokens_ref, gain_ref, routes_ref, group_ref, prob_ref, *outs):
    chunk_refs, weight_ref = outs[:-1], outs[-1]
    experts, slots, width = chunk_refs[0].shape
    rows = tokens_ref.shape[0]
    total = len(chunk_refs) * experts * slots
    widened = tokens_ref[...].astype(jnp.float32)
    mean = jnp.mean(widened * widened, axis=-1, keepdims=True)
    normed = (widened * lax.rsqrt(mean + epsilon) * gain_ref[...]).astype(jnp.bfloat16)
    place = lax.broadcasted_iota(jnp.int32, (total, rows), 0)
    expert = lax.rem(lax.div(place, slots), experts)
    slot = lax.div(place, slots * experts) * slots + lax.rem(place, slots)
    first = routes_ref[0:1, :] == expert
    second = routes_ref[1:2, :] == expert
    named = jnp.where(first, 1.0, jnp.where(second, 1.0, 0.0))
    before = jnp.where(
        lax.broadcasted_iota(jnp.int32, (rows, rows), 0)
        < lax.broadcasted_iota(jnp.int32, (rows, rows), 1),
        1.0,
        0.0,
    )
    rank = jnp.dot(
        named.astype(jnp.bfloat16), before.astype(jnp.bfloat16),
        preferred_element_type=jnp.float32,
    )
    table = jnp.where(rank == slot.astype(jnp.float32), named, 0.0)
    outgoing = jnp.dot(
        table.astype(jnp.bfloat16), normed, preferred_element_type=jnp.float32
    ).astype(jnp.bfloat16)
    for at, chunk_ref in enumerate(chunk_refs):
        chunk_ref[...] = outgoing[at * experts * slots:(at + 1) * experts * slots].reshape(
            experts, slots, width
        )
    prob = prob_ref[...]
    shares = group_ref[...] * prob / jnp.sum(prob, axis=0, keepdims=True)
    weight = table * jnp.where(first, shares[0:1, :], shares[1:2, :])
    high = weight.astype(jnp.bfloat16)
    weight_ref[0] = high
    weight_ref[1] = (weight - high.astype(jnp.float32)).astype(jnp.bfloat16)


def combine_kernel(weight_ref, *refs):
    chunk_refs, out_ref = refs[:-1], refs[-1]
    total = None
    at = 0
    for ref in chunk_refs:
        amount = ref.shape[0] * ref.shape[1]
        returned = ref[...].reshape(amount, ref.shape[2])
        for part in range(2):
            piece = lax.dot_general(
                weight_ref[part, at:at + amount, :], returned, (((0,), (0,)), ((), ())),
                preferred_element_type=jnp.float32,
            )
            total = piece if total is None else total + piece
        at += amount
    out_ref[...] = total.astype(jnp.bfloat16)


def mlp_kernel(rows_ref, *refs):
    weight_refs, out_ref = refs[:-1], refs[-1]
    rows = rows_ref[...].reshape(-1, rows_ref.shape[-1])
    total = None
    for at in range(0, len(weight_refs), 3):
        gate = jnp.dot(rows, weight_refs[at][...], preferred_element_type=jnp.float32)
        up = jnp.dot(rows, weight_refs[at + 1][...], preferred_element_type=jnp.float32)
        hidden = (gate / (1.0 + jnp.exp(-gate)) * up).astype(jnp.bfloat16)
        part = jnp.dot(hidden, weight_refs[at + 2][...], preferred_element_type=jnp.float32)
        total = part if total is None else total + part
    out_ref[...] = total.reshape(out_ref.shape).astype(out_ref.dtype)


def pack_kernel(latent_ref, rope_ref, gain_ref, cos_ref, sin_ref, out_ref):
    width = latent_ref.shape[1]
    widened = latent_ref[...].astype(jnp.float32)
    mean = jnp.mean(widened * widened, axis=-1, keepdims=True)
    out_ref[:, :width] = (
        widened * lax.rsqrt(mean + epsilon) * gain_ref[...]
    ).astype(jnp.bfloat16)
    out_ref[:, width:] = turn(rope_ref[...], cos_ref[...], sin_ref[...])


def attend_kernel(place_ref, query_ref, cos_ref, sin_ref, key_up_ref, value_up_ref, *refs):
    peers = 4
    packed_refs, out_refs, kept_ref = refs[:-peers - 1], refs[-peers - 1:-1], refs[-1]
    own_ep, own_tp, block = place_ref[0], place_ref[1], out_refs[0].shape[0]
    packed = jnp.concatenate([ref[...] for ref in packed_refs], axis=0)
    amount = packed.shape[0]
    latent_width = key_up_ref.shape[0]
    query_rows = query_ref.shape[0]
    heads = query_ref.shape[1] // (NOPE + ROPE_DIM)
    normed, rope = packed[:, :latent_width], packed[:, latent_width:]
    keys = jnp.dot(normed, key_up_ref[...], preferred_element_type=jnp.float32).astype(jnp.bfloat16)
    values = jnp.dot(normed, value_up_ref[...], preferred_element_type=jnp.float32).astype(
        jnp.bfloat16
    )
    column = lax.broadcasted_iota(jnp.int32, (1, amount), 1)
    number = lax.div(column, block)
    ep_of = jnp.full((1, amount), own_ep, jnp.int32)
    steps = (amount // block // peers).bit_length() - 1
    for bit in range(steps):
        taken = lax.bitwise_and(lax.shift_right_logical(number, bit), 1)
        ep_of = lax.bitwise_xor(ep_of, taken * (1 << (steps - 1 - bit)))
    tp_of = jnp.full((1, amount), own_tp, jnp.int32)
    for bit, offset in ((steps, 2), (steps + 1, 1)):
        taken = lax.bitwise_and(lax.shift_right_logical(number, bit), 1)
        tp_of = lax.bitwise_xor(tp_of, taken * offset)
    key_pos = (ep_of * peers + tp_of) * block + lax.rem(column, block)
    query_pos = own_ep * query_rows + lax.broadcasted_iota(jnp.int32, (query_rows, 1), 0)
    allowed = key_pos <= query_pos
    scale = (NOPE + ROPE_DIM) ** (-0.5)
    transposed = (((1,), (1,)), ((), ()))
    for head in range(heads):
        at = head * (NOPE + ROPE_DIM)
        straight = query_ref[:, at:at + NOPE]
        turned = turn(query_ref[:, at + NOPE:at + NOPE + ROPE_DIM], cos_ref[...], sin_ref[...])
        scores = (
            lax.dot_general(
                straight, keys[:, head * NOPE:(head + 1) * NOPE], transposed,
                preferred_element_type=jnp.float32,
            )
            + lax.dot_general(turned, rope, transposed, preferred_element_type=jnp.float32)
        ) * scale
        scores = jnp.where(allowed, scores, masked_value)
        top = jnp.max(scores, axis=-1, keepdims=True)
        raised = jnp.where(allowed, jnp.exp(scores - top), 0.0)
        totals = jnp.sum(raised, axis=-1, keepdims=True)
        weighted = jnp.dot(
            raised.astype(jnp.bfloat16), values[:, head * V_DIM:(head + 1) * V_DIM],
            preferred_element_type=jnp.float32,
        )
        kept_ref[:, head * V_DIM:(head + 1) * V_DIM] = weighted / totals
    for offset, out_ref in enumerate(out_refs):
        start = pl.multiple_of(lax.bitwise_xor(own_tp, offset) * block, block)
        out_ref[...] = kept_ref[pl.ds(start, block), :].astype(jnp.bfloat16)


def project_kernel(place_ref, out_proj_ref, *refs):
    piece_refs, out_ref = refs[:-1], refs[-1]
    total = None
    for offset, ref in enumerate(piece_refs):
        width = ref.shape[1]
        start = pl.multiple_of(lax.bitwise_xor(place_ref[1], offset) * width, width)
        part = jnp.dot(
            ref[...], out_proj_ref[pl.ds(start, width), :], preferred_element_type=jnp.float32
        )
        total = part if total is None else total + part
    out_ref[...] = total.astype(jnp.bfloat16)


VMEM_SPEC = pl.BlockSpec(memory_space=pltpu.VMEM)
SMEM_SPEC = pl.BlockSpec(memory_space=pltpu.SMEM)


def call(kernel, name, shapes, arrays, scalars=0, scratch=()):
    single = not isinstance(shapes, list)
    return pl.pallas_call(
        kernel,
        out_shape=shapes,
        in_specs=[SMEM_SPEC] * scalars + [VMEM_SPEC] * (len(arrays) - scalars),
        out_specs=VMEM_SPEC if single else [VMEM_SPEC] * len(shapes),
        scratch_shapes=list(scratch),
        name=name,
    )(*arrays)


def shape_of(dims, dtype=jnp.bfloat16):
    return jax.ShapeDtypeStruct(dims, dtype)


def doubled(positions):
    cosine, sine = tables(positions, ROPE_DIM)
    return jnp.concatenate([cosine, cosine], axis=1), jnp.concatenate([sine, sine], axis=1)


def mlp(rows, weights, dtype):
    return call(mlp_kernel, "mlp", shape_of(rows.shape, dtype), [rows, *weights])


def fast_body(
    query, latent, rope_key, latent_gain, key_up, value_up, out_proj,
    tokens, moe_gain, routes, group_prob, expert_prob, w_gate, w_up, w_down,
):
    experts = lax.axis_size("ep")
    own_ep = lax.axis_index("ep").astype(jnp.int32)
    own_tp = lax.axis_index("tp").astype(jnp.int32)
    place = jnp.stack([own_ep, own_tp])
    row_count, model_width = tokens.shape
    top_count = routes.shape[1]
    capacity = 2 * top_count * row_count // experts
    chunks = 2
    slots = capacity // chunks

    sent = call(
        dispatch_kernel, "dispatch",
        [shape_of((experts, slots, model_width))] * chunks
        + [shape_of((2, experts * capacity, row_count))],
        [tokens, moe_gain[None, :], routes.T, group_prob[None, :], expert_prob.T],
    )
    outgoing, weight = sent[:-1], sent[-1]
    arrived = [
        lax.all_to_all(part, "ep", split_axis=0, concat_axis=0, tiled=True) for part in outgoing
    ]

    held = (w_gate[0], w_up[0], w_down[0])
    weights = held + tuple(flip(part, "tp", 1) for part in held)

    own_rows = latent.shape[0]
    key_start = (own_ep * 4 + own_tp) * own_rows
    packed = call(
        pack_kernel, "pack", shape_of((own_rows, latent.shape[1] + ROPE_DIM)),
        [latent, rope_key, latent_gain[None, :],
         *doubled(key_start + jnp.arange(own_rows, dtype=jnp.int32))],
    )
    offset = experts // 2
    while offset:
        packed = jnp.concatenate([packed, flip(packed, "ep", offset)], axis=0)
        offset //= 2
    across = flip(packed, "tp", 2)
    partner = flip(jnp.concatenate([packed, across], axis=0), "tp", 1)
    query_rows = query.shape[0]
    query_pos = own_ep * query_rows + jnp.arange(query_rows, dtype=jnp.int32)
    width = key_up.shape[1]
    pieces = call(
        attend_kernel, "attend", [shape_of((own_rows, width))] * 4,
        [place, query, *doubled(query_pos), key_up, value_up, packed, across, partner],
        scalars=1, scratch=[pltpu.VMEM((query_rows, width), jnp.float32)],
    )
    pieces = [pieces[0]] + [flip(pieces[t], "tp", t) for t in (1, 2, 3)]
    mixed = call(
        project_kernel, "project", shape_of((own_rows, model_width)),
        [place, out_proj, *pieces], scalars=1,
    )

    returned = []
    for mine in arrived:
        theirs = flip(mine, "tp", 2)
        back = flip(mlp(theirs, weights, jnp.bfloat16), "tp", 2)
        own = mlp(mine, weights, jnp.float32)
        final = (own + back.astype(jnp.float32)).astype(jnp.bfloat16)
        returned.append(lax.all_to_all(final, "ep", split_axis=0, concat_axis=0, tiled=True))
    moe_out = call(
        combine_kernel, "combine", shape_of((row_count, model_width)), [weight, *returned]
    )
    return (mixed, moe_out)


def wide_body(
    query, latent, rope_key, latent_gain, key_up, value_up, out_proj,
    tokens, moe_gain, routes, group_prob, expert_prob, w_gate, w_up, w_down,
):
    experts = lax.axis_size("ep")
    capacity = 2 * routes.shape[1] * tokens.shape[0] // experts
    everything = lax.all_gather(
        pack_latent(latent, rope_key, latent_gain), ("ep", "tp"), axis=0, tiled=True
    )
    query_rows = query.shape[0]
    query_pos = lax.axis_index("ep") * query_rows + jnp.arange(query_rows, dtype=jnp.int32)
    key_pos = jnp.arange(everything.shape[0], dtype=jnp.int32)
    attention = attend(query, everything, key_pos, query_pos, key_up, value_up)
    own_attention = lax.all_to_all(attention, "tp", split_axis=0, concat_axis=1, tiled=True)
    mixed = jnp.dot(own_attention, out_proj, preferred_element_type=jnp.float32).astype(
        jnp.bfloat16
    )

    row_count, model_width = tokens.shape
    top_count = routes.shape[1]
    normed = rms_scale(tokens, moe_gain).astype(jnp.bfloat16)
    flat_routes = routes.reshape(-1)
    onehot = (flat_routes[:, None] == jnp.arange(experts, dtype=jnp.int32)[None, :]).astype(
        jnp.int32
    )
    earlier = jnp.cumsum(onehot, axis=0) - onehot
    slot_index = jnp.sum(earlier * onehot, axis=1)
    target = flat_routes * capacity + slot_index
    owner = target[None, :] == jnp.arange(experts * capacity, dtype=jnp.int32)[:, None]
    table = jnp.any(owner.reshape(experts * capacity, row_count, top_count), axis=2).astype(
        jnp.bfloat16
    )
    outgoing = jnp.dot(table, normed, preferred_element_type=jnp.float32).astype(jnp.bfloat16)
    outgoing = outgoing.reshape(experts, capacity, model_width)
    arrived = lax.all_to_all(outgoing, "ep", split_axis=0, concat_axis=0, tiled=True)
    flat_rows = arrived.reshape(experts * capacity, model_width)
    shard_rows = lax.all_gather(flat_rows, "tp", axis=0, tiled=True)
    gate_values = jnp.dot(shard_rows, w_gate[0], preferred_element_type=jnp.float32)
    up_values = jnp.dot(shard_rows, w_up[0], preferred_element_type=jnp.float32)
    hidden = (jax.nn.silu(gate_values) * up_values).astype(jnp.bfloat16)
    partial = jnp.dot(hidden, w_down[0], preferred_element_type=jnp.float32).astype(jnp.bfloat16)
    summed = lax.psum_scatter(partial, "tp", scatter_dimension=0, tiled=True)
    result = summed.reshape(experts, capacity, model_width)
    returned = lax.all_to_all(result, "ep", split_axis=0, concat_axis=0, tiled=True)
    returned_flat = returned.reshape(experts * capacity, model_width)
    picked = returned_flat[target].reshape(row_count, top_count, model_width).astype(jnp.float32)
    shares = group_prob[:, None] * expert_prob / jnp.sum(expert_prob, axis=1, keepdims=True)
    return (mixed, jnp.sum(shares[:, :, None] * picked, axis=1).astype(jnp.bfloat16))


def solution(mesh):
    experts, parts = mesh.shape["ep"], mesh.shape["tp"]
    unrolled = experts in (2, 4, 8, 16) and parts == 4
    return jax.shard_map(
        fast_body if unrolled else wide_body,
        mesh=mesh,
        in_specs=(
            P("ep", "tp"),
            P(("ep", "tp"), None),
            P(("ep", "tp"), None),
            P(),
            P(None, "tp"),
            P(None, "tp"),
            P(),
            P(("ep", "tp"), None),
            P(),
            P(("ep", "tp"), None),
            P(("ep", "tp")),
            P(("ep", "tp"), None),
            P("ep", None, "tp"),
            P("ep", None, "tp"),
            P("ep", "tp", None),
        ),
        out_specs=(P(("ep", "tp"), None), P(("ep", "tp"), None)),
        check_vma=False,
    )
```

```python
import jax
import jax.numpy as jnp
from jax import lax
from jax.experimental import pallas as pl
from jax.experimental.pallas import tpu as pltpu
from jax.sharding import PartitionSpec as P


NOPE = 64
ROPE_DIM = 32
V_DIM = 64


epsilon = 1e-06
rope_base = 10000.0
masked_value = -1e30


def rms_scale(values, gain):
    widened = values.astype(jnp.float32)
    return widened * lax.rsqrt(jnp.mean(widened * widened, axis=-1, keepdims=True) + epsilon) * gain


def tables(positions, rope_width):
    half_width = rope_width // 2
    inverse = rope_base ** (-2.0 * jnp.arange(half_width, dtype=jnp.float32) / rope_width)
    angles = positions.astype(jnp.float32)[:, None] * inverse[None, :]
    return (jnp.cos(angles), jnp.sin(angles))


def rotate(values, cosine, sine):
    half_width = values.shape[-1] // 2
    lower = values[..., :half_width]
    upper = values[..., half_width:]
    return jnp.concatenate([lower * cosine - upper * sine, lower * sine + upper * cosine], axis=-1)


def flip(value, axis, offset):
    count = lax.axis_size(axis)
    return lax.ppermute(value, axis, [(i, i ^ offset) for i in range(count)])


def attend(query, packed, key_pos, query_pos, key_up, value_up):
    query_rows = query.shape[0]
    head_count = query.shape[1] // (NOPE + ROPE_DIM)
    latent_width = key_up.shape[0]
    query_cos, query_sin = tables(query_pos, ROPE_DIM)
    query_heads = query.reshape(query_rows, head_count, NOPE + ROPE_DIM)
    turned = rotate(
        query_heads[..., NOPE:].astype(jnp.float32), query_cos[:, None, :], query_sin[:, None, :]
    ).astype(jnp.bfloat16)
    query_rot = jnp.concatenate([query_heads[..., :NOPE], turned], axis=-1)
    normed = packed[:, :latent_width]
    rope_part = packed[:, latent_width:]
    keys = jnp.dot(normed, key_up, preferred_element_type=jnp.float32).astype(jnp.bfloat16)
    values = jnp.dot(normed, value_up, preferred_element_type=jnp.float32).astype(jnp.bfloat16)
    allowed = key_pos[None, :] <= query_pos[:, None]
    scale = (NOPE + ROPE_DIM) ** (-0.5)
    pieces = []
    for head in range(head_count):
        full_keys = jnp.concatenate([keys[:, head * NOPE:(head + 1) * NOPE], rope_part], axis=1)
        scores = lax.dot_general(
            query_rot[:, head], full_keys, (((1,), (1,)), ((), ())),
            preferred_element_type=jnp.float32,
        ) * scale
        scores = jnp.where(allowed, scores, masked_value)
        top = jnp.max(scores, axis=-1, keepdims=True)
        raised = jnp.where(allowed, jnp.exp(scores - top), 0.0)
        totals = jnp.sum(raised, axis=-1, keepdims=True)
        weighted = jnp.dot(
            raised.astype(jnp.bfloat16), values[:, head * V_DIM:(head + 1) * V_DIM],
            preferred_element_type=jnp.float32,
        )
        pieces.append((weighted / totals).astype(jnp.bfloat16))
    return jnp.concatenate(pieces, axis=1)


def pack_latent(latent, rope_key, latent_gain):
    own_rows = latent.shape[0]
    start = (lax.axis_index("ep") * lax.axis_size("tp") + lax.axis_index("tp")) * own_rows
    normed = rms_scale(latent, latent_gain).astype(jnp.bfloat16)
    cosine, sine = tables(start + jnp.arange(own_rows, dtype=jnp.int32), ROPE_DIM)
    rotated = rotate(rope_key.astype(jnp.float32), cosine, sine).astype(jnp.bfloat16)
    return jnp.concatenate([normed, rotated], axis=1)


def rotation(start, rows):
    half = ROPE_DIM // 2
    column = lax.broadcasted_iota(jnp.int32, (1, ROPE_DIM), 1)
    inverse = jnp.zeros((1, ROPE_DIM), jnp.float32)
    for at in range(half):
        own = jnp.logical_or(column == at, column == at + half)
        inverse = jnp.where(own, rope_base ** (-2.0 * at / ROPE_DIM), inverse)
    position = start + lax.broadcasted_iota(jnp.int32, (rows, 1), 0)
    angles = position.astype(jnp.float32) * inverse
    return jnp.cos(angles), jnp.sin(angles)


def turn(values, cosine, sine):
    width = values.shape[-1]
    half = width // 2
    row = lax.broadcasted_iota(jnp.int32, (width, width), 0)
    column = lax.broadcasted_iota(jnp.int32, (width, width), 1)
    swap = jnp.where(column < half, column + half, column - half) == row
    sign = jnp.where(column < half, -1.0, 1.0)
    swapped = jnp.dot(
        values, jnp.where(swap, sign, 0.0).astype(jnp.bfloat16),
        preferred_element_type=jnp.float32,
    )
    return (values.astype(jnp.float32) * cosine + swapped * sine).astype(jnp.bfloat16)


def pick(values, count, width, skip):
    group = values.shape[1] // count
    row = lax.broadcasted_iota(jnp.int32, (values.shape[1], count * width), 0)
    column = lax.broadcasted_iota(jnp.int32, (values.shape[1], count * width), 1)
    chosen = row == lax.div(column, width) * group + skip + lax.rem(column, width)
    return jnp.dot(
        values, jnp.where(chosen, 1.0, 0.0).astype(jnp.bfloat16),
        preferred_element_type=jnp.float32,
    )


def pack_kernel(
    place_ref, latent_ref, rope_ref, latent_gain_ref, routes_ref, group_ref, prob_ref,
    out_ref, facts_ref,
):
    rows, width = latent_ref.shape
    widened = latent_ref[...].astype(jnp.float32)
    mean = jnp.mean(widened * widened, axis=-1, keepdims=True)
    out_ref[:, :width] = (
        widened * lax.rsqrt(mean + epsilon) * latent_gain_ref[...]
    ).astype(jnp.bfloat16)
    cosine, sine = rotation((place_ref[0] * 4 + place_ref[1]) * rows, rows)
    out_ref[:, width:] = turn(rope_ref[...], cosine, sine)
    prob = prob_ref[...]
    facts_ref[0:2] = routes_ref[...].astype(jnp.float32)
    facts_ref[2:4] = group_ref[...] * prob / jnp.sum(prob, axis=0, keepdims=True)
    facts_ref[4:8] = jnp.zeros((4, facts_ref.shape[1]), jnp.float32)


def dispatch_kernel(place_ref, gain_ref, *refs):
    (own_ref, other_ref, own_facts_ref, other_facts_ref), outs = refs[:4], refs[4:]
    chunk_refs, weight_ref = outs[:-1], outs[-1]
    span = chunk_refs[0].shape[0]
    capacity = span // 2
    rows = own_ref.shape[0]
    total = len(chunk_refs) * span
    widened = jnp.concatenate([own_ref[...], other_ref[...]], axis=0).astype(jnp.float32)
    mean = jnp.mean(widened * widened, axis=-1, keepdims=True)
    normed = (widened * lax.rsqrt(mean + epsilon) * gain_ref[...]).astype(jnp.bfloat16)
    facts = jnp.concatenate([own_facts_ref[...], other_facts_ref[...]], axis=1)
    place = lax.broadcasted_iota(jnp.int32, (total, 2 * rows), 0)
    token = lax.broadcasted_iota(jnp.int32, (total, 2 * rows), 1)
    number = lax.div(place, span)
    expert = jnp.zeros((total, 2 * rows), jnp.int32)
    for at in range(len(chunk_refs)):
        expert = jnp.where(number == at, place_ref[2 + at], expert)
    slot = lax.rem(place, capacity)
    same = lax.rem(lax.div(place, capacity), 2) == lax.div(token, rows)
    first = facts[0:1] == expert.astype(jnp.float32)
    second = facts[1:2] == expert.astype(jnp.float32)
    named = jnp.where(jnp.logical_and(same, jnp.logical_or(first, second)), 1.0, 0.0)
    before = jnp.where(
        lax.broadcasted_iota(jnp.int32, (2 * rows, 2 * rows), 0)
        < lax.broadcasted_iota(jnp.int32, (2 * rows, 2 * rows), 1),
        1.0,
        0.0,
    )
    rank = jnp.dot(
        named.astype(jnp.bfloat16), before.astype(jnp.bfloat16),
        preferred_element_type=jnp.float32,
    )
    table = jnp.where(rank == slot.astype(jnp.float32), named, 0.0)
    outgoing = jnp.dot(
        table.astype(jnp.bfloat16), normed, preferred_element_type=jnp.float32
    ).astype(jnp.bfloat16)
    for at, chunk_ref in enumerate(chunk_refs):
        chunk_ref[...] = outgoing[at * span:(at + 1) * span]
    weight = table * jnp.where(first, facts[2:3], facts[3:4])
    high = weight.astype(jnp.bfloat16)
    weight_ref[0] = high
    weight_ref[1] = (weight - high.astype(jnp.float32)).astype(jnp.bfloat16)


def combine_kernel(weight_ref, *refs):
    chunk_refs, own_ref, other_ref = refs[:-2], refs[-2], refs[-1]
    returned = jnp.concatenate([ref[...] for ref in chunk_refs], axis=0)
    total = None
    for part in range(2):
        piece = lax.dot_general(
            weight_ref[part], returned, (((0,), (0,)), ((), ())),
            preferred_element_type=jnp.float32,
        )
        total = piece if total is None else total + piece
    rows = own_ref.shape[0]
    own_ref[...] = total[:rows]
    other_ref[...] = total[rows:].astype(jnp.bfloat16)


def mlp_kernel(*refs):
    count = (len(refs) - 6) // 2
    row_refs, weight_refs, out_refs = refs[:count], refs[count:-count], refs[-count:]
    rows = jnp.concatenate([ref[...] for ref in row_refs], axis=0)
    total = None
    for at in range(0, len(weight_refs), 3):
        gate = jnp.dot(rows, weight_refs[at][...], preferred_element_type=jnp.float32)
        up = jnp.dot(rows, weight_refs[at + 1][...], preferred_element_type=jnp.float32)
        hidden = (gate / (1.0 + jnp.exp(-gate)) * up).astype(jnp.bfloat16)
        part = jnp.dot(hidden, weight_refs[at + 2][...], preferred_element_type=jnp.float32)
        total = part if total is None else total + part
    amount = out_refs[0].shape[0]
    for at, out_ref in enumerate(out_refs):
        out_ref[...] = total[at * amount:(at + 1) * amount].astype(jnp.bfloat16)


def attend_kernel(place_ref, query_ref, key_up_ref, value_up_ref, *refs):
    peers = 4
    packed_refs, out_refs = refs[:peers], refs[peers:2 * peers]
    kept_ref, packed_ref, copied = refs[2 * peers:]
    part = packed_refs[0].shape[0]
    copies = [
        pltpu.make_async_copy(ref, packed_ref.at[pl.ds(at * part, part)], copied.at[at])
        for at, ref in enumerate(packed_refs)
    ]
    for copy in copies:
        copy.start()
    cosine, sine = rotation(place_ref[0] * query_ref.shape[0], query_ref.shape[0])
    for copy in copies:
        copy.wait()
    own_ep, own_tp, block = place_ref[0], place_ref[1], out_refs[0].shape[0]
    packed = packed_ref[...]
    amount = packed.shape[0]
    latent_width = key_up_ref.shape[0]
    query_rows = query_ref.shape[0]
    heads = query_ref.shape[1] // (NOPE + ROPE_DIM)
    normed, rope = packed[:, :latent_width], packed[:, latent_width:]
    keys = jnp.dot(normed, key_up_ref[...], preferred_element_type=jnp.float32).astype(jnp.bfloat16)
    values = jnp.dot(normed, value_up_ref[...], preferred_element_type=jnp.float32).astype(
        jnp.bfloat16
    )
    column = lax.broadcasted_iota(jnp.int32, (1, amount), 1)
    number = lax.div(column, block)
    ep_of = jnp.full((1, amount), own_ep, jnp.int32)
    tp_of = jnp.full((1, amount), own_tp, jnp.int32)
    steps = (amount // block // peers).bit_length() - 1
    offsets = [(2, 0)] + [(0, 1 << bit) for bit in reversed(range(steps))] + [(1, 0)]
    for bit, (tp_offset, ep_offset) in enumerate(offsets):
        taken = lax.bitwise_and(lax.shift_right_logical(number, bit), 1)
        ep_of = lax.bitwise_xor(ep_of, taken * ep_offset)
        tp_of = lax.bitwise_xor(tp_of, taken * tp_offset)
    key_pos = (ep_of * peers + tp_of) * block + lax.rem(column, block)
    stacked = heads * query_rows
    row = lax.broadcasted_iota(jnp.int32, (stacked, 1), 0)
    query_pos = own_ep * query_rows + lax.rem(row, query_rows)
    width = heads * NOPE
    straight = pick(query_ref[...], heads, NOPE, 0)
    lane = lax.broadcasted_iota(jnp.int32, (1, width), 1)
    own_lanes = lax.div(row, query_rows) == lax.div(lane, NOPE)
    straight = jnp.where(own_lanes, jnp.concatenate([straight] * heads, axis=0), 0.0).astype(
        jnp.bfloat16
    )
    turned = jnp.concatenate(
        [
            turn(query_ref[:, at + NOPE:at + NOPE + ROPE_DIM], cosine, sine)
            for at in range(0, query_ref.shape[1], NOPE + ROPE_DIM)
        ],
        axis=0,
    )
    transposed = (((1,), (1,)), ((), ()))
    scores = (
        lax.dot_general(straight, keys, transposed, preferred_element_type=jnp.float32)
        + lax.dot_general(turned, rope, transposed, preferred_element_type=jnp.float32)
    ) * (NOPE + ROPE_DIM) ** (-0.5)
    scores = jnp.where(key_pos <= query_pos, scores, masked_value)
    top = jnp.max(scores, axis=-1, keepdims=True)
    raised = jnp.exp(scores - top)
    totals = jnp.sum(raised, axis=-1, keepdims=True)
    weighted = jnp.dot(raised.astype(jnp.bfloat16), values, preferred_element_type=jnp.float32)
    weighted = jnp.where(own_lanes, weighted / totals, 0.0)
    kept_ref[...] = sum(
        weighted[head * query_rows:(head + 1) * query_rows] for head in range(heads)
    )
    for offset, out_ref in enumerate(out_refs):
        start = pl.multiple_of(lax.bitwise_xor(own_tp, offset) * block, block)
        out_ref[...] = kept_ref[pl.ds(start, block), :].astype(jnp.bfloat16)


def project_kernel(place_ref, out_proj_ref, *refs):
    piece_refs, out_ref = refs[:-1], refs[-1]
    total = None
    for offset, ref in enumerate(piece_refs):
        width = ref.shape[1]
        start = pl.multiple_of(lax.bitwise_xor(place_ref[1], offset) * width, width)
        part = jnp.dot(
            ref[...], out_proj_ref[pl.ds(start, width), :], preferred_element_type=jnp.float32
        )
        total = part if total is None else total + part
    out_ref[...] = total.astype(jnp.bfloat16)


VMEM_SPEC = pl.BlockSpec(memory_space=pltpu.VMEM)
HBM_SPEC = pl.BlockSpec(memory_space=pltpu.MemorySpace.HBM)
SMEM_SPEC = pl.BlockSpec(memory_space=pltpu.SMEM)


def call(kernel, shapes, arrays, scalars=0, scratch=(), far=0):
    single = not isinstance(shapes, list)
    specs = [SMEM_SPEC] * scalars + [VMEM_SPEC] * (len(arrays) - scalars - far)
    return pl.pallas_call(
        kernel,
        out_shape=shapes,
        in_specs=specs + [HBM_SPEC] * far,
        out_specs=VMEM_SPEC if single else [VMEM_SPEC] * len(shapes),
        scratch_shapes=list(scratch),
    )(*arrays)


def shape_of(dims, dtype=jnp.bfloat16):
    return jax.ShapeDtypeStruct(dims, dtype)


def add_rows(near, back):
    return (near.astype(jnp.float32) + back.astype(jnp.float32)).astype(jnp.bfloat16)


def fast_body(*arguments):
    return fast_layer(*arguments)


def fast_layer(
    query, latent, rope_key, latent_gain, key_up, value_up, out_proj,
    tokens, moe_gain, routes, group_prob, expert_prob, w_gate, w_up, w_down,
):
    experts = lax.axis_size("ep")
    own_ep = lax.axis_index("ep").astype(jnp.int32)
    own_tp = lax.axis_index("tp").astype(jnp.int32)
    offsets = offsets_of(experts)
    steps = range(len(offsets[0]))
    core = jnp.bitwise_and(own_tp, 1)
    place = jnp.stack(
        [own_ep, own_tp]
        + [own_ep ^ jnp.where(core == 0, offsets[0][i], offsets[1][i]) for i in steps]
    )
    row_count, model_width = tokens.shape
    capacity = 2 * routes.shape[1] * row_count // experts

    other_tokens = flip(tokens, "tp", 1)
    own_rows = latent.shape[0]
    packed, facts = call(
        pack_kernel,
        [shape_of((own_rows, latent.shape[1] + ROPE_DIM)), shape_of((8, row_count), jnp.float32)],
        [place, latent, rope_key, latent_gain[None, :], routes.T, group_prob[None, :],
         expert_prob.T], 1,
    )
    other_facts = flip(facts, "tp", 1)
    sent = call(
        dispatch_kernel,
        [shape_of((2 * capacity, model_width))] * len(steps)
        + [shape_of((2, 2 * len(steps) * capacity, 2 * row_count))],
        [place, moe_gain[None, :], tokens, other_tokens, facts, other_facts], 1,
    )
    outgoing, weight = sent[:-1], sent[-1]
    mine = [shift(outgoing[i], offsets, i) for i in steps]
    theirs = [flip(mine[i], "tp", 2) for i in steps]

    held = (w_gate[0], w_up[0], w_down[0])
    weights = held + tuple(flip(part, "tp", 1) for part in held)

    across = flip(packed, "tp", 2)
    packed = jnp.concatenate([packed, across], 0)
    offset = experts // 2
    while offset > 1:
        more = flip(packed, "ep", offset)
        packed = jnp.concatenate([packed, more], 0)
        offset //= 2
    beside = flip(packed, "ep", 1)
    partners = [flip(packed, "tp", 1), flip(beside, "tp", 1)]
    query_rows = query.shape[0]
    width = key_up.shape[1]
    pieces = call(
        attend_kernel, [shape_of((own_rows, width))] * 4,
        [place, query, key_up, value_up, packed, beside, *partners],
        1,
        [pltpu.VMEM((query_rows, width), jnp.float32),
         pltpu.VMEM((4 * packed.shape[0], packed.shape[1]), jnp.bfloat16),
         pltpu.SemaphoreType.DMA((4,))],
        4,
    )
    pieces = [pieces[0]] + [flip(pieces[t], "tp", t) for t in (1, 2, 3)]
    mixed = call(
        project_kernel, shape_of((own_rows, model_width)),
        [place, out_proj, *pieces], 1,
    )

    rows = shape_of((2 * capacity, model_width))
    near, far = {}, {}
    for near_steps, far_steps in CALLS:
        lots = [mine[i] for i in near_steps] + [theirs[i] for i in far_steps]
        parts = call(mlp_kernel, [rows] * len(lots), lots + list(weights))
        near.update(zip(near_steps, parts))
        far.update(zip(far_steps, parts[len(near_steps):]))
    returned = []
    for i in steps:
        back = flip(far[i], "tp", 2)
        final = add_rows(near[i], back)
        returned.append(shift(final, offsets, i))
    own, other = call(
        combine_kernel,
        [shape_of((row_count, model_width), jnp.float32), shape_of((row_count, model_width))],
        [weight, *returned],
    )
    other = flip(other, "tp", 1)
    moe_out = add_rows(own, other)
    return (mixed, moe_out)


def offsets_of(experts):
    half = experts // 2
    return ((0, half, 2, half + 1), (1, half + 2, 3, half + 3))


def shift(value, offsets, step):
    parts = lax.axis_size("tp")
    table = [
        (e * parts + t, (e ^ offsets[t % 2][step]) * parts + t)
        for e in range(lax.axis_size("ep")) for t in range(parts)
    ]
    return lax.ppermute(value, ("ep", "tp"), table)


CALLS = (((0, 1), (0,)), ((2,), (1, 2)), ((3,), (3,)))


def wide_body(
    query, latent, rope_key, latent_gain, key_up, value_up, out_proj,
    tokens, moe_gain, routes, group_prob, expert_prob, w_gate, w_up, w_down,
):
    experts = lax.axis_size("ep")
    capacity = 2 * routes.shape[1] * tokens.shape[0] // experts
    everything = lax.all_gather(
        pack_latent(latent, rope_key, latent_gain), ("ep", "tp"), axis=0, tiled=True
    )
    query_rows = query.shape[0]
    query_pos = lax.axis_index("ep") * query_rows + jnp.arange(query_rows, dtype=jnp.int32)
    key_pos = jnp.arange(everything.shape[0], dtype=jnp.int32)
    attention = attend(query, everything, key_pos, query_pos, key_up, value_up)
    own_attention = lax.all_to_all(attention, "tp", split_axis=0, concat_axis=1, tiled=True)
    mixed = jnp.dot(own_attention, out_proj, preferred_element_type=jnp.float32).astype(
        jnp.bfloat16
    )

    row_count, model_width = tokens.shape
    top_count = routes.shape[1]
    normed = rms_scale(tokens, moe_gain).astype(jnp.bfloat16)
    flat_routes = routes.reshape(-1)
    onehot = (flat_routes[:, None] == jnp.arange(experts, dtype=jnp.int32)[None, :]).astype(
        jnp.int32
    )
    earlier = jnp.cumsum(onehot, axis=0) - onehot
    slot_index = jnp.sum(earlier * onehot, axis=1)
    target = flat_routes * capacity + slot_index
    owner = target[None, :] == jnp.arange(experts * capacity, dtype=jnp.int32)[:, None]
    table = jnp.any(owner.reshape(experts * capacity, row_count, top_count), axis=2).astype(
        jnp.bfloat16
    )
    outgoing = jnp.dot(table, normed, preferred_element_type=jnp.float32).astype(jnp.bfloat16)
    outgoing = outgoing.reshape(experts, capacity, model_width)
    arrived = lax.all_to_all(outgoing, "ep", split_axis=0, concat_axis=0, tiled=True)
    flat_rows = arrived.reshape(experts * capacity, model_width)
    shard_rows = lax.all_gather(flat_rows, "tp", axis=0, tiled=True)
    gate_values = jnp.dot(shard_rows, w_gate[0], preferred_element_type=jnp.float32)
    up_values = jnp.dot(shard_rows, w_up[0], preferred_element_type=jnp.float32)
    hidden = (jax.nn.silu(gate_values) * up_values).astype(jnp.bfloat16)
    partial = jnp.dot(hidden, w_down[0], preferred_element_type=jnp.float32).astype(jnp.bfloat16)
    summed = lax.psum_scatter(partial, "tp", scatter_dimension=0, tiled=True)
    result = summed.reshape(experts, capacity, model_width)
    returned = lax.all_to_all(result, "ep", split_axis=0, concat_axis=0, tiled=True)
    returned_flat = returned.reshape(experts * capacity, model_width)
    picked = returned_flat[target].reshape(row_count, top_count, model_width).astype(jnp.float32)
    shares = group_prob[:, None] * expert_prob / jnp.sum(expert_prob, axis=1, keepdims=True)
    return (mixed, jnp.sum(shares[:, :, None] * picked, axis=1).astype(jnp.bfloat16))


def solution(mesh):
    experts, parts = mesh.shape["ep"], mesh.shape["tp"]
    unrolled = experts == 8 and parts == 4
    return jax.shard_map(
        fast_body if unrolled else wide_body,
        mesh=mesh,
        in_specs=(
            P("ep", "tp"),
            P(("ep", "tp"), None),
            P(("ep", "tp"), None),
            P(),
            P(None, "tp"),
            P(None, "tp"),
            P(),
            P(("ep", "tp"), None),
            P(),
            P(("ep", "tp"), None),
            P(("ep", "tp")),
            P(("ep", "tp"), None),
            P("ep", None, "tp"),
            P("ep", None, "tp"),
            P("ep", "tp", None),
        ),
        out_specs=(P(("ep", "tp"), None), P(("ep", "tp"), None)),
        check_vma=False,
    )
```
